32 devices in a mesh: fs: 8 (over z, y), tp: 4 (over x, core).
Axes of the slice: x: 2, y: 2, z: 4, core: 2. Of those that a mesh axis runs over, the one named last changes fastest.
Arguments:
- query_latent_rows: bfloat16 [12288, 1024], P('fs'), may hold values from -6 to 6
- grad_q: bfloat16 [12288, 3072], P('fs', 'tp'), may hold values from -6 to 6
- head_out: bfloat16 [12288, 2048], P('fs', 'tp'), may hold values from -6 to 6
- grad_out: bfloat16 [12288, 4096], P('fs'), may hold values from -6 to 6
- proj_q: bfloat16 [1024, 256], P('fs'), may hold values from -0.5 to 0.5
- proj_o: bfloat16 [4096, 256], P('fs'), may hold values from -0.5 to 0.5
- query_up_weight: float32 [1024, 3072], P('fs', 'tp'), may hold values from -0.1875 to 0.1875
- weight_o: float32 [4096, 2048], P('fs', 'tp'), may hold values from -0.125 to 0.125
- first_q: float32 [256, 3072], P('fs', 'tp'), may hold values from -6 to 6
- second_q: float32 [256, 3072], P('fs', 'tp'), may hold values from 0.25 to 4
- first_o: float32 [256, 2048], P('fs', 'tp'), may hold values from -6 to 6
- second_o: float32 [256, 2048], P('fs', 'tp'), may hold values from 0.25 to 4
Outputs:
- new_weight_q: float32 [1024, 3072], P('fs', 'tp')
- new_weight_o: float32 [4096, 2048], P('fs', 'tp')
- new_first_q: float32 [256, 3072], P('fs', 'tp')
- new_second_q: float32 [256, 3072], P('fs', 'tp')
- new_first_o: float32 [256, 2048], P('fs', 'tp')
- new_second_o: float32 [256, 2048], P('fs', 'tp')
- step_q: float32 [1024, 3072], P('fs', 'tp')
- step_o: float32 [4096, 2048], P('fs', 'tp')
- copy_q: bfloat16 [1024, 3072], P(None, 'tp')
- copy_o: bfloat16 [4096, 2048], P(None, 'tp')
The draws below stay inside these ranges and needn't reach their ends.
All inputs are finite; a program needn't handle non-finite values.
Results may differ from the reference program's by a relative error of at most 0.008.
Values may be sent and summed in bfloat16 or wider, within the bound.
A program may use at most 128 MiB of HBM per device.

```python
import math
import jax
import jax.numpy as jnp
from jax import lax

D = 4096
QUERY_LATENT = 1024
RANK = 256
QUERY_COLUMNS = 3072
BW = 2048
TOKEN_TOTAL = 12288


def reduced_basis(key, height):
    column = jnp.arange(RANK, dtype=jnp.float32)
    falloff = 10.0 ** (-column / RANK)
    entries = jnp.clip(jax.random.normal(key, (height, RANK), jnp.float32), -4.0, 4.0)
    return (entries * falloff[None, :] / math.sqrt(height)).astype(jnp.bfloat16)


def draw_proj_q(key, part):
    return reduced_basis(jax.random.fold_in(key, 11), QUERY_LATENT)


def draw_proj_o(key, part):
    return reduced_basis(jax.random.fold_in(key, 12), D)


def raised(drawn, stream_key, source, target, shards_of, factor):
    def block_of(axis_at):
        return (jnp.arange(drawn.shape[axis_at]) // (drawn.shape[axis_at] // shards_of)).reshape((-1,) + (1,) * (drawn.ndim - 1 - axis_at))

    one_side = jax.random.permutation(stream_key, shards_of)[block_of(target)]
    far = (block_of(target) + shards_of // 2) % shards_of
    return jnp.where((block_of(source) == one_side) | (block_of(source) == far), factor * drawn, drawn)


def steps_of(key, extent, cuts, smallest, largest):
    loudness, own = 1.0, jax.random.fold_in(key, 6)
    for axis_at, shards_of in cuts:
        heights = jnp.exp(jax.random.uniform(jax.random.fold_in(own, axis_at), (shards_of,), jnp.float32, smallest / len(cuts), largest / len(cuts)))
        loudness = loudness * jnp.repeat(heights, extent[axis_at] // shards_of).reshape([-1 if axis == axis_at else 1 for axis in range(len(extent))])
    return loudness


def scatter_about(stream_key, shape, deviation, most, split=(), held_as=jnp.bfloat16):
    array = deviation * jax.random.normal(stream_key, shape, jnp.float32)
    if split:
        array = array * steps_of(stream_key, shape, split, -0.22, 0.18)
    return jnp.clip(array, -most, most).astype(held_as)


def noise_with(rng, shape, spread, limit, pieces, heavy, held_as=jnp.bfloat16):
    result = spread * jax.random.normal(rng, shape, jnp.float32)
    if pieces:
        result = result * steps_of(rng, shape, pieces, -0.22, 0.18)
    return jnp.clip(raised(result, jax.random.fold_in(rng, 3), *heavy), -limit, limit).astype(held_as)


def setup_inputs(seed: int = 0) -> dict:
    streams_of = jax.random.split(jax.random.key(seed), 13)
    query_latent_rows = noise_with(streams_of[0], (TOKEN_TOTAL, QUERY_LATENT), 1.0, 6.0, ((0, 8),), (0, 1, 8, 2.0))
    grad_q = scatter_about(streams_of[1], (TOKEN_TOTAL, QUERY_COLUMNS), 1.0, 6.0, ((0, 8), (1, 4)))
    head_out = scatter_about(streams_of[2], (TOKEN_TOTAL, BW), 1.0, 6.0, ((0, 8), (1, 4)))
    grad_out = noise_with(streams_of[3], (TOKEN_TOTAL, D), 1.0, 6.0, ((0, 8),), (0, 1, 8, 2.0))
    proj_q = draw_proj_q(jax.random.fold_in(streams_of[12], 71), 0)
    proj_o = draw_proj_o(jax.random.fold_in(streams_of[12], 71), 0)
    query_up_weight = scatter_about(streams_of[6], (QUERY_LATENT, QUERY_COLUMNS), QUERY_LATENT ** -0.5, 0.1875, ((0, 8), (1, 4)), jnp.float32)
    weight_o = scatter_about(streams_of[7], (D, BW), BW ** -0.5, 0.125, ((0, 8), (1, 4)), jnp.float32)
    first_q = scatter_about(streams_of[8], (RANK, QUERY_COLUMNS), 1.0, 6.0, ((0, 8), (1, 4)), jnp.float32)
    second_q = jnp.clip(jnp.exp(math.log(4.0) - 2.7725887 * jax.random.uniform(streams_of[9], (RANK, QUERY_COLUMNS), jnp.float32) ** steps_of(streams_of[9], (RANK, QUERY_COLUMNS), ((0, 8), (1, 4)), -0.2, 0.2)), 0.25, 4.0)
    first_o = scatter_about(streams_of[10], (RANK, BW), 1.0, 6.0, ((0, 8), (1, 4)), jnp.float32)
    second_o = jnp.clip(jnp.exp(math.log(4.0) - 2.7725887 * jax.random.uniform(streams_of[11], (RANK, BW), jnp.float32) ** steps_of(streams_of[11], (RANK, BW), ((0, 8), (1, 4)), -0.2, 0.2)), 0.25, 4.0)
    return dict(query_latent_rows=query_latent_rows, grad_q=grad_q, head_out=head_out, grad_out=grad_out, proj_q=proj_q, proj_o=proj_o, query_up_weight=query_up_weight, weight_o=weight_o, first_q=first_q, second_q=second_q, first_o=first_o, second_o=second_o)


beta_first = 0.8
beta_second = 0.9
epsilon = 1e-08
decay_rate = 2.0
step_rate = 0.05

def moments(first, second, reduced, clip_scale):
    scaled = clip_scale * reduced
    first_new = beta_first * first + (1.0 - beta_first) * scaled
    second_new = beta_second * second + (1.0 - beta_second) * scaled * scaled
    return (first_new, second_new, first_new / (jnp.sqrt(second_new) + epsilon))

def reference(query_latent_rows, grad_q, head_out, grad_out, proj_q, proj_o, query_up_weight, weight_o, first_q, second_q, first_o, second_o):
    highest = lax.Precision.HIGHEST
    grad_full_q = jnp.dot(query_latent_rows.T, grad_q, preferred_element_type=jnp.float32)
    grad_full_o = jnp.dot(grad_out.T, head_out, preferred_element_type=jnp.float32)
    basis_q = proj_q.astype(jnp.float32)
    basis_o = proj_o.astype(jnp.float32)
    low_q = jnp.dot(basis_q.T, grad_full_q, precision=highest, preferred_element_type=jnp.float32)
    low_o = jnp.dot(basis_o.T, grad_full_o, precision=highest, preferred_element_type=jnp.float32)
    sum_squares = jnp.sum(low_q * low_q) + jnp.sum(low_o * low_o)
    target = math.sqrt(RANK * (QUERY_COLUMNS + BW))
    clip_scale = jnp.minimum(1.0, target / jnp.sqrt(sum_squares))
    first_nq, second_nq, direct_q = moments(first_q, second_q, low_q, clip_scale)
    first_no, second_no, direct_o = moments(first_o, second_o, low_o, clip_scale)
    step_q = jnp.dot(basis_q, direct_q, precision=highest, preferred_element_type=jnp.float32) + decay_rate * query_up_weight
    step_o = jnp.dot(basis_o, direct_o, precision=highest, preferred_element_type=jnp.float32) + decay_rate * weight_o
    new_weight_q = query_up_weight - step_rate * step_q
    new_weight_o = weight_o - step_rate * step_o
    return (new_weight_q, new_weight_o, first_nq, second_nq, first_no, second_no, step_q, step_o, new_weight_q.astype(jnp.bfloat16), new_weight_o.astype(jnp.bfloat16))
```

```python
import functools
import math

import jax
import jax.numpy as jnp
from jax import lax
from jax.experimental import pallas as pl
from jax.experimental.pallas import tpu as pltpu
from jax.sharding import PartitionSpec as P

beta_first = 0.8
beta_second = 0.9
epsilon = 1e-08
decay_rate = 2.0
step_rate = 0.05
f32 = jnp.float32
bf16 = jnp.bfloat16
MESH = pl.DeviceIdType.MESH


def moments(first, second, scaled):
    first_new = beta_first * first + (1.0 - beta_first) * scaled
    second_new = beta_second * second + (1.0 - beta_second) * scaled * scaled
    return (first_new, second_new, first_new / (jnp.sqrt(second_new) + epsilon))


def kernel(
    n,
    tps,
    s,
    entries,
    tile,
    ql_hbm,
    gq_hbm,
    ho_hbm,
    go_hbm,
    pq_in,
    po_in,
    wq_in,
    wo_in,
    first_in,
    second_in,
    wq_all,
    wo_all,
    pq_all,
    po_all,
    dir_all,
    scaled_out,
    ql,
    gq,
    ho,
    go,
    tq,
    to,
    low_send,
    low_recv,
    dir_own,
    ss_fs,
    ss_tp,
    ss_own,
    load_sem,
    p1_send,
    p1_recv,
    p2_send,
    p2_recv,
    w_send,
    w_recv,
    rs_send,
    rs_recv,
    sf_send,
    sf_recv,
    st_send,
    st_recv,
    d_send,
    d_recv,
):
    f = lax.axis_index("fs")
    t = lax.axis_index("tp")
    fs_peer = [lax.rem(f + k, n) for k in range(n)]
    fs_from = [lax.rem(f + n - k, n) for k in range(n)]
    tp_peer = [lax.rem(t + k, tps) for k in range(tps)]
    tp_from = [lax.rem(t + tps - k, tps) for k in range(tps)]
    mine = lax.rem(t, s)
    group = t - mine

    loads = [
        pltpu.make_async_copy(src, dst, load_sem.at[i])
        for i, (src, dst) in enumerate(((go_hbm, go), (ho_hbm, ho), (ql_hbm, ql), (gq_hbm, gq)))
    ]
    for load in loads:
        load.start()

    barrier = pltpu.get_barrier_semaphore()
    for k in range(1, n):
        pl.semaphore_signal(barrier, inc=1, device_id=(fs_peer[k], t), device_id_type=MESH)
    for k in range(1, tps):
        pl.semaphore_signal(barrier, inc=1, device_id=(f, tp_peer[k]), device_id_type=MESH)
    pl.semaphore_wait(barrier, n + tps - 2)

    def send(src, dst, send_sem, recv_sem, device):
        copy = pltpu.make_async_remote_copy(
            src_ref=src,
            dst_ref=dst,
            send_sem=send_sem,
            recv_sem=recv_sem,
            device_id=device,
            device_id_type=MESH,
        )
        copy.start()
        return copy

    pairs = ((pq_in, pq_all), (po_in, po_all))
    first_hop = []
    for k in range(1, n):
        first_hop.append(
            [
                send(own.at[mine], whole.at[f, mine], p1_send.at[i, k], p1_recv.at[i, k], (fs_peer[k], t))
                for i, (own, whole) in enumerate(pairs)
            ]
        )

    depth = min(4, n)
    width = n // depth
    row, column = f // width, lax.rem(f, width)
    place = column * depth + row + lax.rem(column, 2) * (depth - 1 - 2 * row)

    def at_place(p):
        p = lax.rem(p + 2 * n, n)
        y = p // depth
        r = lax.rem(p, depth)
        return (r + lax.rem(y, 2) * (depth - 1 - 2 * r)) * width + y

    weights = ((wq_in, wq_all), (wo_in, wo_all))
    ring = []

    def ring_step(step):
        if step > 0:
            for copy in ring[step - 1]:
                copy.wait_recv()
        if step > n - 2:
            return
        copies = []
        for i, (own, whole) in enumerate(weights):
            half = own.shape[0] // 2
            for way, sign in enumerate((1, -1)):
                rows = pl.ds(way * half, half)
                owner = at_place(place - sign * step)
                source = own.at[rows] if step == 0 else whole.at[owner, rows]
                copies.append(
                    send(
                        source,
                        whole.at[owner, rows],
                        w_send.at[step, i, way],
                        w_recv.at[step, i, way],
                        (at_place(place + sign), t),
                    )
                )
        ring.append(copies)

    ring_step(0)
    for own, whole in weights + pairs:
        whole[f] = own[...]

    second_hop = []
    for k in range(1, n):
        for copy in first_hop[k - 1]:
            copy.wait_recv()
        for j in range(1, s):
            target = group + lax.rem(mine + j, s)
            for i, (own, whole) in enumerate(pairs):
                slot = whole.at[fs_from[k], mine]
                second_hop.append(
                    send(slot, slot, p2_send.at[i, k, j], p2_recv.at[i, k, j], (f, target))
                )
    for load in loads:
        load.wait()
    for copy in second_hop:
        copy.wait_recv()
    ring_step(1)

    tokens = go.shape[0]
    ro = po_all.shape[2] * s
    rank = pq_all.shape[3]

    @pl.loop(0, tokens // tile)
    def _(i):
        at = pl.ds(pl.multiple_of(i * tile, tile), tile)
        acc = jnp.zeros((tile, rank), f32)
        for b in range(n):
            acc += jnp.dot(
                go[at, b * ro : (b + 1) * ro],
                po_all[b].reshape(ro, rank),
                preferred_element_type=f32,
            )
        to[:, at] = acc.T.astype(bf16)
        acc = jnp.dot(ql[at, :], pq_all[...].reshape(-1, rank), preferred_element_type=f32)
        tq[:, at] = acc.T.astype(bf16)

    cq = gq.shape[1]
    co = ho.shape[1]
    rr = low_send.shape[1]
    for left, right, base in ((tq, gq, 0), (to, ho, cq)):
        for c in range(0, right.shape[1], 128):
            part = jnp.dot(left[...], right[:, c : c + 128], preferred_element_type=f32)
            low_send[:, :, base + c : base + c + 128] = part.astype(bf16).reshape(n, rr, 128)

    scatter = [
        send(low_send.at[fs_peer[k]], low_recv.at[f], rs_send.at[k], rs_recv.at[k], (fs_peer[k], t))
        for k in range(1, n)
    ]
    low_recv[f] = low_send[f]
    ring_step(2)
    for copy in scatter:
        copy.wait_recv()
    low = low_recv[0].astype(f32)
    for b in range(1, n):
        low += low_recv[b].astype(f32)
    ss_own[...] = jnp.broadcast_to(jnp.sum(low * low, keepdims=True), ss_own.shape)
    sums = [
        send(ss_own, ss_fs.at[f], sf_send.at[k], sf_recv.at[k], (fs_peer[k], t)) for k in range(1, n)
    ]
    ss_fs[f] = ss_own[...]
    for copy in sums:
        copy.wait_recv()
    ss_tp[t] = jnp.sum(ss_fs[...], axis=0)
    sums_tp = [
        send(ss_tp.at[t], ss_tp.at[t], st_send.at[k], st_recv.at[k], (f, tp_peer[k]))
        for k in range(1, tps)
    ]
    ring_step(3)
    for copy in sums_tp:
        copy.wait_recv()
    total = jnp.sum(ss_tp[...], axis=0)[0:1, 0:1]
    clip_scale = jnp.minimum(1.0, math.sqrt(entries) / jnp.sqrt(total))
    scaled = clip_scale * low
    scaled_out[...] = scaled
    _, _, direct = moments(first_in[...], second_in[...], scaled)
    dir_own[...] = direct.astype(bf16)
    spread = [
        send(dir_own, dir_all.at[f], d_send.at[k], d_recv.at[k], (fs_peer[k], t)) for k in range(1, n)
    ]
    dir_all[f] = dir_own[...]
    for step in range(4, n):
        ring_step(step)
    for copy in spread:
        copy.wait_recv()
    for group_of in (*first_hop, second_hop, *ring, scatter, sums, sums_tp, spread):
        for copy in group_of:
            copy.wait_send()


def per_device(
    n,
    tps,
    query_latent_rows,
    grad_q,
    head_out,
    grad_out,
    proj_q,
    proj_o,
    query_up_weight,
    weight_o,
    first_q,
    second_q,
    first_o,
    second_o,
):
    rq, rank = proj_q.shape
    ro = proj_o.shape[0]
    cq, co = grad_q.shape[1], head_out.shape[1]
    rr = first_q.shape[0]
    tokens = grad_out.shape[0]
    columns = cq + co
    s = math.gcd(tps, rq // 16)
    tile = math.gcd(tokens, 256)
    entries = rr * n * columns * tps
    first = jnp.concatenate([first_q, first_o], axis=1)
    second = jnp.concatenate([second_q, second_o], axis=1)
    wq = query_up_weight.astype(bf16)
    wo = weight_o.astype(bf16)
    vmem = pl.BlockSpec(memory_space=pltpu.VMEM)
    hbm = pl.BlockSpec(memory_space=pl.ANY)
    dma = pltpu.SemaphoreType.DMA
    wq_all, wo_all, pq_all, po_all, dir_all, scaled = pl.pallas_call(
        functools.partial(kernel, n, tps, s, entries, tile),
        out_shape=(
            jax.ShapeDtypeStruct((n, rq, cq), bf16),
            jax.ShapeDtypeStruct((n, ro, co), bf16),
            jax.ShapeDtypeStruct((n, s, rq // s, rank), bf16),
            jax.ShapeDtypeStruct((n, s, ro // s, rank), bf16),
            jax.ShapeDtypeStruct((n, rr, columns), bf16),
            jax.ShapeDtypeStruct((rr, columns), f32),
        ),
        in_specs=[hbm] * 4 + [vmem] * 6,
        out_specs=(vmem,) * 6,
        scratch_shapes=[
            pltpu.VMEM(query_latent_rows.shape, bf16),
            pltpu.VMEM(grad_q.shape, bf16),
            pltpu.VMEM(head_out.shape, bf16),
            pltpu.VMEM(grad_out.shape, bf16),
            pltpu.VMEM((rank, tokens), bf16),
            pltpu.VMEM((rank, tokens), bf16),
            pltpu.VMEM((n, rr, columns), bf16),
            pltpu.VMEM((n, rr, columns), bf16),
            pltpu.VMEM((rr, columns), bf16),
            pltpu.VMEM((n, 8, 128), f32),
            pltpu.VMEM((tps, 8, 128), f32),
            pltpu.VMEM((8, 128), f32),
            dma((4,)),
            dma((2, n)),
            dma((2, n)),
            dma((2, n, s)),
            dma((2, n, s)),
            dma((n - 1, 2, 2)),
            dma((n - 1, 2, 2)),
            dma((n,)),
            dma((n,)),
            dma((n,)),
            dma((n,)),
            dma((tps,)),
            dma((tps,)),
            dma((n,)),
            dma((n,)),
        ],
        compiler_params=pltpu.CompilerParams(
            collective_id=0, has_side_effects=True, vmem_limit_bytes=60 * 1024 * 1024
        ),
    )(
        query_latent_rows,
        grad_q,
        head_out,
        grad_out,
        proj_q.reshape(s, rq // s, rank),
        proj_o.reshape(s, ro // s, rank),
        wq,
        wo,
        first,
        second,
    )
    direct = dir_all.reshape(rank, columns)
    direct_q, direct_o = direct[:, :cq], direct[:, cq:]
    first_nq, second_nq, _ = moments(first_q, second_q, scaled[:, :cq])
    first_no, second_no, _ = moments(first_o, second_o, scaled[:, cq:])

    def update(basis, directions, weight):
        step = jnp.dot(basis, directions, preferred_element_type=f32) + decay_rate * weight
        return step, weight - step_rate * step

    step_q, new_weight_q = update(proj_q, direct_q, query_up_weight)
    step_o, new_weight_o = update(proj_o, direct_o, weight_o)
    _, copy_q = update(pq_all.reshape(n * rq, rank), direct_q, wq_all.reshape(n * rq, cq).astype(f32))
    _, copy_o = update(po_all.reshape(n * ro, rank), direct_o, wo_all.reshape(n * ro, co).astype(f32))
    return (
        new_weight_q,
        new_weight_o,
        first_nq,
        second_nq,
        first_no,
        second_no,
        step_q,
        step_o,
        copy_q.astype(bf16),
        copy_o.astype(bf16),
    )


def solution(mesh):
    both = P("fs", "tp")
    rows = P("fs", None)
    return jax.shard_map(
        functools.partial(per_device, mesh.shape["fs"], mesh.shape["tp"]),
        mesh=mesh,
        in_specs=(rows, both, both, rows, rows, rows) + (both,) * 6,
        out_specs=(both,) * 8 + (P(None, "tp"),) * 2,
        check_vma=False,
    )
```

```python
import functools
import math

import jax
import jax.numpy as jnp
from jax import lax
from jax.experimental import pallas as pl
from jax.experimental.pallas import tpu as pltpu
from jax.sharding import PartitionSpec as P

beta_first = 0.8
beta_second = 0.9
epsilon = 1e-08
decay_rate = 2.0
step_rate = 0.05
f32 = jnp.float32
bf16 = jnp.bfloat16
MESH = pl.DeviceIdType.MESH


def moments(first, second, scaled):
    first_new = beta_first * first + (1.0 - beta_first) * scaled
    second_new = beta_second * second + (1.0 - beta_second) * scaled * scaled
    return (first_new, second_new, first_new / (jnp.sqrt(second_new) + epsilon))


def kernel(
    n,
    tps,
    s,
    entries,
    tile,
    ql_hbm,
    gq_hbm,
    ho_hbm,
    go_hbm,
    pq_in,
    po_in,
    wq_in,
    wo_in,
    first_q,
    second_q,
    first_o,
    second_o,
    wq_all,
    wo_all,
    pq_all,
    po_all,
    dir_all,
    scaled_out,
    ql,
    gq,
    ho,
    go,
    tq,
    to,
    low_send,
    low_y,
    z_send,
    z_recv,
    ss_fs,
    ss_tp,
    ss_own,
    load_sem,
    a_send,
    a_recv,
    b_send,
    b_recv,
    c_send,
    c_recv,
    w_send,
    w_recv,
    ry_send,
    ry_recv,
    rz_send,
    rz_recv,
    sf_send,
    sf_recv,
    st_send,
    st_recv,
    da_send,
    da_recv,
    db_send,
    db_recv,
):
    f = lax.axis_index("fs")
    t = lax.axis_index("tp")
    depth = min(4, n)
    width = n // depth
    z, y = f // width, lax.rem(f, width)

    def fs_at(kz, ky):
        return lax.rem(z + kz + depth, depth) * width + lax.rem(y + ky + width, width)

    mine = lax.rem(t, s)
    group = t - mine

    loads = [
        pltpu.make_async_copy(src, dst, load_sem.at[i])
        for i, (src, dst) in enumerate(((go_hbm, go), (ho_hbm, ho), (ql_hbm, ql), (gq_hbm, gq)))
    ]
    for load in loads:
        load.start()

    barrier = pltpu.get_barrier_semaphore()
    for k in range(1, n):
        pl.semaphore_signal(barrier, inc=1, device_id=(lax.rem(f + k, n), t), device_id_type=MESH)
    for k in range(1, tps):
        pl.semaphore_signal(barrier, inc=1, device_id=(f, lax.rem(t + k, tps)), device_id_type=MESH)
    wq_all[f] = wq_in[...].astype(bf16)
    wo_all[f] = wo_in[...].astype(bf16)
    pl.semaphore_wait(barrier, n + tps - 2)
    started = []

    def send(src, dst, send_sem, recv_sem, device):
        copy = pltpu.make_async_remote_copy(
            src_ref=src,
            dst_ref=dst,
            send_sem=send_sem,
            recv_sem=recv_sem,
            device_id=device,
            device_id_type=MESH,
        )
        copy.start()
        started.append(copy)
        return copy

    pairs = ((pq_in, pq_all), (po_in, po_all))
    along_z = {}
    for k in range(1, depth):
        along_z[k] = [
            send(own.at[mine], whole.at[f, mine], a_send.at[i, k], a_recv.at[i, k], (fs_at(k, 0), t))
            for i, (own, whole) in enumerate(pairs)
        ]
    along_y = {}

    def pass_y(kz):
        for ky in range(1, width):
            copies = []
            for i, (own, whole) in enumerate(pairs):
                slot = whole.at[fs_at(-kz, 0), mine]
                source = own.at[mine] if kz == 0 else slot
                copies.append(
                    send(source, slot, b_send.at[i, kz, ky], b_recv.at[i, kz, ky], (fs_at(0, ky), t))
                )
            along_y[kz, ky] = copies

    along_tp = []

    def pass_tp(kz, ky):
        for j in range(1, s):
            target = group + lax.rem(mine + j, s)
            for i, (own, whole) in enumerate(pairs):
                slot = whole.at[fs_at(-kz, -ky), mine]
                at = kz * width + ky
                along_tp.append(
                    send(slot, slot, c_send.at[i, at, j], c_recv.at[i, at, j], (f, target))
                )

    pass_y(0)

    place = y * depth + z + lax.rem(y, 2) * (depth - 1 - 2 * z)

    def at_place(p):
        p = lax.rem(p + 2 * n, n)
        py = p // depth
        r = lax.rem(p, depth)
        return (r + lax.rem(py, 2) * (depth - 1 - 2 * r)) * width + py

    parts = []
    for whole, pieces in ((wq_all, 1), (wo_all, 2)):
        half = whole.shape[1] // 2
        for piece in range(pieces):
            for way, sign in enumerate((1, -1)):
                size = half // pieces
                parts.append((whole, pl.ds(way * half + piece * size, size), sign))
    ring = []

    def ring_step(step):
        copies = []
        for i, (whole, rows, sign) in enumerate(parts):
            if step > 0:
                ring[step - 1][i].wait_recv()
            if step < n - 1:
                slot = whole.at[at_place(place - sign * step), rows]
                copies.append(
                    send(slot, slot, w_send.at[step, i], w_recv.at[step, i], (at_place(place + sign), t))
                )
        ring.append(copies)

    ring_step(0)
    for own, whole in pairs:
        whole[f] = own[...]

    for kz in range(1, depth):
        for copy in along_z[kz]:
            copy.wait_recv()
        pass_y(kz)
        pass_tp(kz, 0)
    for kz in range(depth):
        for ky in range(1, width):
            for copy in along_y[kz, ky]:
                copy.wait_recv()
            pass_tp(kz, ky)
    for load in loads:
        load.wait()
    for copy in along_tp:
        copy.wait_recv()
    ring_step(1)

    tokens = go.shape[0]
    ro = po_all.shape[2] * s
    rank = pq_all.shape[3]

    @pl.loop(0, tokens // tile)
    def _(i):
        at = pl.ds(pl.multiple_of(i * tile, tile), tile)
        acc = jnp.zeros((tile, rank), f32)
        for b in range(n):
            acc += jnp.dot(
                go[at, b * ro : (b + 1) * ro],
                po_all[b].reshape(ro, rank),
                preferred_element_type=f32,
            )
        to[:, at] = acc.T.astype(bf16)
        acc = jnp.dot(ql[at, :], pq_all[...].reshape(-1, rank), preferred_element_type=f32)
        tq[:, at] = acc.T.astype(bf16)

    cq = gq.shape[1]
    rr = low_send.shape[2]
    for left, right, base in ((tq, gq, 0), (to, ho, cq)):
        for c in range(0, right.shape[1], 128):
            part = jnp.dot(left[...], right[:, c : c + 128], preferred_element_type=f32)
            part = part.astype(bf16).reshape(depth, width, rr, 128)
            for b in range(width):
                low_send[b, :, :, base + c : base + c + 128] = part[:, b]

    sums_y = [
        send(
            low_send.at[lax.rem(y + k, width)],
            low_y.at[k],
            ry_send.at[k],
            ry_recv.at[k],
            (fs_at(0, k), t),
        )
        for k in range(1, width)
    ]
    ring_step(2)
    for copy in sums_y:
        copy.wait_recv()
    for b in range(depth):
        z_sum = low_send[y, b].astype(f32)
        for k in range(1, width):
            z_sum += low_y[k, b].astype(f32)
        z_send[b] = z_sum.astype(bf16)
    sums_z = [
        send(
            z_send.at[lax.rem(z + k, depth)],
            z_recv.at[k],
            rz_send.at[k],
            rz_recv.at[k],
            (fs_at(k, 0), t),
        )
        for k in range(1, depth)
    ]
    low = z_send[z].astype(f32)
    for copy in sums_z:
        copy.wait_recv()
    for k in range(1, depth):
        low += z_recv[k].astype(f32)
    ss_own[...] = jnp.broadcast_to(jnp.sum(low * low, keepdims=True), ss_own.shape)
    sums = [
        send(ss_own, ss_fs.at[f], sf_send.at[k], sf_recv.at[k], (lax.rem(f + k, n), t))
        for k in range(1, n)
    ]
    ss_fs[f] = ss_own[...]
    ring_step(3)
    for copy in sums:
        copy.wait_recv()
    ss_tp[t] = jnp.sum(ss_fs[...], axis=0)
    sums_tp = [
        send(ss_tp.at[t], ss_tp.at[t], st_send.at[k], st_recv.at[k], (f, lax.rem(t + k, tps)))
        for k in range(1, tps)
    ]
    for copy in sums_tp:
        copy.wait_recv()
    total = jnp.sum(ss_tp[...], axis=0)[0:1, 0:1]
    clip_scale = jnp.minimum(1.0, math.sqrt(entries) / jnp.sqrt(total))
    scaled = clip_scale * low
    scaled_out[...] = scaled
    _, _, direct = moments(first_q[...], second_q[...], scaled[:, :cq])
    dir_all[f, :, :cq] = direct.astype(bf16)
    _, _, direct = moments(first_o[...], second_o[...], scaled[:, cq:])
    dir_all[f, :, cq:] = direct.astype(bf16)

    spread = {
        k: send(dir_all.at[f], dir_all.at[f], da_send.at[k], da_recv.at[k], (fs_at(k, 0), t))
        for k in range(1, depth)
    }
    spread_y = []

    def spread_on(kz):
        slot = dir_all.at[fs_at(-kz, 0)]
        for ky in range(1, width):
            spread_y.append(
                send(slot, slot, db_send.at[kz, ky], db_recv.at[kz, ky], (fs_at(0, ky), t))
            )

    spread_on(0)
    ring_step(4)
    for k in range(1, depth):
        spread[k].wait_recv()
        spread_on(k)
    for step in range(5, n):
        ring_step(step)
    for copy in spread_y:
        copy.wait_recv()
    for copy in started:
        copy.wait_send()


def finish(
    wq_all,
    wo_all,
    pq_all,
    po_all,
    dir_all,
    scaled,
    proj_q,
    proj_o,
    weight_q,
    weight_o,
    first_q,
    second_q,
    first_o,
    second_o,
    new_weight_q,
    new_weight_o,
    first_nq,
    second_nq,
    first_no,
    second_no,
    step_q,
    step_o,
    copy_q,
    copy_o,
):
    cq = copy_q.shape[1]
    rank = proj_q.shape[1]
    direct = dir_all[...].reshape(rank, dir_all.shape[2])
    sides = ((direct[:, :cq], wq_all, pq_all, copy_q), (direct[:, cq:], wo_all, po_all, copy_o))

    def update(basis, directions, weight):
        step = jnp.dot(basis, directions, preferred_element_type=f32) + decay_rate * weight
        return step, weight - step_rate * step

    for directions, weights, bases, copy in sides:
        _, new = update(bases[0].reshape(-1, rank), directions, weights[0].astype(f32))
        copy[...] = new.astype(bf16)

    @pl.when(pl.program_id(0) == 0)
    def _():
        step_q[...], new_weight_q[...] = update(proj_q[...], direct[:, :cq], weight_q[...])
        step_o[...], new_weight_o[...] = update(proj_o[...], direct[:, cq:], weight_o[...])
        first_nq[...], second_nq[...], _ = moments(first_q[...], second_q[...], scaled[:, :cq])
        first_no[...], second_no[...], _ = moments(first_o[...], second_o[...], scaled[:, cq:])


def per_device(
    n,
    tps,
    query_latent_rows,
    grad_q,
    head_out,
    grad_out,
    proj_q,
    proj_o,
    query_up_weight,
    weight_o,
    first_q,
    second_q,
    first_o,
    second_o,
):
    rq, rank = proj_q.shape
    ro = proj_o.shape[0]
    cq, co = grad_q.shape[1], head_out.shape[1]
    rr = first_q.shape[0]
    tokens = grad_out.shape[0]
    columns = cq + co
    s = math.gcd(tps, rq // 16)
    depth = min(4, n)
    width = n // depth
    tile = math.gcd(tokens, 256)
    entries = rr * n * columns * tps
    vmem = pl.BlockSpec(memory_space=pltpu.VMEM)
    hbm = pl.BlockSpec(memory_space=pl.ANY)
    dma = pltpu.SemaphoreType.DMA

    def both(*shape):
        return [dma(shape), dma(shape)]

    own = (first_q, second_q, first_o, second_o)
    gathered = pl.pallas_call(
        functools.partial(kernel, n, tps, s, entries, tile),
        out_shape=(
            jax.ShapeDtypeStruct((n, rq, cq), bf16),
            jax.ShapeDtypeStruct((n, ro, co), bf16),
            jax.ShapeDtypeStruct((n, s, rq // s, rank), bf16),
            jax.ShapeDtypeStruct((n, s, ro // s, rank), bf16),
            jax.ShapeDtypeStruct((n, rr, columns), bf16),
            jax.ShapeDtypeStruct((rr, columns), f32),
        ),
        in_specs=[hbm] * 4 + [vmem] * 8,
        out_specs=(vmem,) * 6,
        scratch_shapes=[
            pltpu.VMEM(query_latent_rows.shape, bf16),
            pltpu.VMEM(grad_q.shape, bf16),
            pltpu.VMEM(head_out.shape, bf16),
            pltpu.VMEM(grad_out.shape, bf16),
            pltpu.VMEM((rank, tokens), bf16),
            pltpu.VMEM((rank, tokens), bf16),
            pltpu.VMEM((width, depth, rr, columns), bf16),
            pltpu.VMEM((width, depth, rr, columns), bf16),
            pltpu.VMEM((depth, rr, columns), bf16),
            pltpu.VMEM((depth, rr, columns), bf16),
            pltpu.VMEM((n, 8, 128), f32),
            pltpu.VMEM((tps, 8, 128), f32),
            pltpu.VMEM((8, 128), f32),
            dma((4,)),
            *both(2, depth),
            *both(2, depth, width),
            *both(2, n, s),
            *both(n - 1, 6),
            *both(width),
            *both(depth),
            *both(n),
            *both(tps),
            *both(depth),
            *both(depth, width),
        ],
        compiler_params=pltpu.CompilerParams(
            collective_id=0, has_side_effects=True, vmem_limit_bytes=60 * 1024 * 1024
        ),
    )(
        query_latent_rows,
        grad_q,
        head_out,
        grad_out,
        proj_q.reshape(s, rq // s, rank),
        proj_o.reshape(s, ro // s, rank),
        query_up_weight,
        weight_o,
        *own,
    )

    def whole(shape):
        return pl.BlockSpec(shape, lambda i: (0,) * len(shape))

    def rows_of(shape):
        return pl.BlockSpec((1, *shape[1:]), lambda i: (i,) + (0,) * (len(shape) - 1))

    held = (proj_q, proj_o, query_up_weight, weight_o, *own)
    outs = (query_up_weight, weight_o, first_q, second_q, first_o, second_o, query_up_weight, weight_o)
    return pl.pallas_call(
        finish,
        grid=(n,),
        out_shape=tuple(jax.ShapeDtypeStruct(a.shape, f32) for a in outs)
        + (jax.ShapeDtypeStruct((n * rq, cq), bf16), jax.ShapeDtypeStruct((n * ro, co), bf16)),
        in_specs=[rows_of(a.shape) for a in gathered[:4]]
        + [whole(a.shape) for a in (*gathered[4:], *held)],
        out_specs=tuple(whole(a.shape) for a in outs)
        + (pl.BlockSpec((rq, cq), lambda i: (i, 0)), pl.BlockSpec((ro, co), lambda i: (i, 0))),
        compiler_params=pltpu.CompilerParams(vmem_limit_bytes=48 * 1024 * 1024),
    )(*gathered, *held)


def solution(mesh):
    both = P("fs", "tp")
    rows = P("fs", None)
    return jax.shard_map(
        functools.partial(per_device, mesh.shape["fs"], mesh.shape["tp"]),
        mesh=mesh,
        in_specs=(rows, both, both, rows, rows, rows) + (both,) * 6,
        out_specs=(both,) * 8 + (P(None, "tp"),) * 2,
        check_vma=False,
    )
```
